32 devices in a mesh: sp: 8 (over z, y), tp: 4 (over x, core).
Axes of the slice: x: 2, y: 2, z: 4, core: 2. Of those that a mesh axis runs over, the one named last changes fastest.
Arguments:
- values_in: bfloat16 [4, 8192, 1024], P(None, 'sp', 'tp'), may hold values from -6 to 6
- gates_in: bfloat16 [4, 8192, 1024], P(None, 'sp', 'tp'), may hold values from -8 to 8
- conv_taps: bfloat16 [31, 1024], P(None, 'tp'), may hold values from -3 to 3
- conv_bias: bfloat16 [1024], P('tp'), may hold values from -3 to 3
- norm_gain: bfloat16 [1024], P('tp'), may hold values from 0.099609375 to 1.8984375
- out_weight: bfloat16 [1024, 4096], P('tp'), may hold values from -0.1875 to 0.1875
- out_grad: bfloat16 [4, 8192, 4096], P(None, 'sp'), may hold values from -1.5 to 1.5
Outputs:
- values_grad: bfloat16 [4, 8192, 1024], P(None, 'sp', 'tp')
- gates_grad: bfloat16 [4, 8192, 1024], P(None, 'sp', 'tp')
- taps_grad: float32 [31, 1024], P(None, 'tp')
- gain_grad: float32 [1024], P('tp')
- bias_grad: float32 [1024], P('tp')
- weight_grad: float32 [1024, 4096], P(('tp', 'sp'))
The draws below stay inside these ranges and needn't reach their ends.
All inputs are finite; a program needn't handle non-finite values.
Results may differ from the reference program's by a relative error of at most 0.0048.
Values may be sent and summed in bfloat16 or wider, within the bound.
A program may use at most 128 MiB of HBM per device.

```python
import jax
import jax.numpy as jnp
from jax import lax

D = 4096
C = 1024
K = 31
SEQS = 4
TOKENS = 8192


def draw_conv_taps(key, part):
    normal_key, scale_key = jax.random.split(jax.random.fold_in(key, 7))
    group_count = C // 64
    scales = jnp.exp(jax.random.uniform(scale_key, (group_count,), jnp.float32, -1.2, 1.2))
    scales = jnp.repeat(scales, 64)
    noise = jax.random.normal(normal_key, (K, C), jnp.float32)
    noise = jnp.clip(noise, -4.0, 4.0)
    return (noise * scales[None, :] * K ** (-0.5)).astype(jnp.bfloat16)


def block_levels(key, shape, cuts, smallest, largest):
    def one(dim, blocks):
        draws = jax.random.uniform(jax.random.fold_in(jax.random.fold_in(key, 6), dim), (blocks,), jnp.float32, smallest / len(cuts), largest / len(cuts))
        return jnp.repeat(jnp.exp(draws), shape[dim] // blocks).reshape((-1,) + (1,) * (len(shape) - dim - 1))

    level = one(*cuts[0])
    for cut in cuts[1:]:
        level = level * one(*cut)
    return level


def normal_values(key, shape, spread, reach, cuts=(), held_as=jnp.bfloat16):
    level = block_levels(key, shape, cuts, -0.22, 0.18) if cuts else 1.0
    result = jax.random.normal(key, shape, jnp.float32) * spread * level
    return jnp.minimum(jnp.maximum(result, -reach), reach).astype(held_as)


def setup_inputs(seed: int = 0) -> dict:
    key_of = jax.random.split(jax.random.key(seed), 8)
    values_in = normal_values(key_of[0], (SEQS, TOKENS, C), 1.0, 6.0, ((1, 8), (2, 4)))
    gates_in = normal_values(key_of[1], (SEQS, TOKENS, C), 1.5, 8.0, ((1, 8), (2, 4)))
    conv_taps = draw_conv_taps(jax.random.fold_in(key_of[7], 71), 0)
    conv_bias = normal_values(key_of[3], (C,), 0.5, 3.0, ((0, 4),))
    norm_gain = jnp.clip(1.0 + 0.18 * jax.random.normal(key_of[4], (C,), jnp.float32), 0.099609375, 1.8984375).astype(jnp.bfloat16)
    out_weight = normal_values(key_of[5], (C, D), C ** -0.5, 0.1875, ((0, 4),))
    out_grad = normal_values(key_of[6], (SEQS, TOKENS, D), 0.25, 1.5, ((1, 8),))
    return {"values_in": values_in, "gates_in": gates_in, "conv_taps": conv_taps, "conv_bias": conv_bias, "norm_gain": norm_gain, "out_weight": out_weight, "out_grad": out_grad}


EPS = 1e-05

def reference(values_in, gates_in, conv_taps, conv_bias, norm_gain, out_weight, out_grad):
    sig = jax.nn.sigmoid(gates_in.astype(jnp.float32))
    gated = (values_in.astype(jnp.float32) * sig).astype(jnp.bfloat16)
    tap_rows = conv_taps.astype(jnp.float32)
    length = gated.shape[1]
    padded = jnp.pad(gated.astype(jnp.float32), ((0, 0), (K - 1, 0), (0, 0)))
    conv = jnp.zeros(gated.shape, jnp.float32) + conv_bias.astype(jnp.float32)
    for tap_index in range(K):
        conv = conv + tap_rows[tap_index] * padded[:, tap_index:tap_index + length]
    channel_mean = lax.optimization_barrier(jnp.mean(conv, axis=-1, keepdims=True))
    centered = conv - channel_mean
    variance = lax.optimization_barrier(jnp.mean(centered * centered, axis=-1, keepdims=True))
    inverse = lax.rsqrt(variance + EPS)
    normed = centered * inverse
    gain = norm_gain.astype(jnp.float32)
    scaled = normed * gain
    swished = jax.nn.silu(scaled).astype(jnp.bfloat16)
    flat_grad = out_grad.reshape(-1, D)
    weight_grad = jnp.dot(swished.reshape(-1, C).T, flat_grad, preferred_element_type=jnp.float32)
    swish_grad = jnp.dot(flat_grad, out_weight.T, preferred_element_type=jnp.float32).reshape(gated.shape)
    scaled_sig = jax.nn.sigmoid(scaled)
    scaled_grad = swish_grad * scaled_sig * (1.0 + scaled * (1.0 - scaled_sig))
    gain_grad = lax.optimization_barrier(jnp.sum(scaled_grad * normed, axis=(0, 1)))
    normed_grad = scaled_grad * gain
    conv_grad = inverse * (normed_grad - lax.optimization_barrier(jnp.mean(normed_grad, axis=-1, keepdims=True)) - normed * lax.optimization_barrier(jnp.mean(normed_grad * normed, axis=-1, keepdims=True)))
    bias_grad = lax.optimization_barrier(jnp.sum(conv_grad, axis=(0, 1)))
    taps_grad = jnp.stack([lax.optimization_barrier(jnp.sum(conv_grad * padded[:, tap_index:tap_index + length], axis=(0, 1))) for tap_index in range(K)])
    padded_grad = jnp.pad(conv_grad, ((0, 0), (0, K - 1), (0, 0)))
    gated_grad = jnp.zeros(gated.shape, jnp.float32)
    for tap_index in range(K):
        begin = K - 1 - tap_index
        gated_grad = gated_grad + tap_rows[tap_index] * padded_grad[:, begin:begin + length]
    values_grad = (gated_grad * sig).astype(jnp.bfloat16)
    gates_grad = (gated_grad * values_in.astype(jnp.float32) * sig * (1.0 - sig)).astype(jnp.bfloat16)
    return (values_grad, gates_grad, taps_grad, gain_grad, bias_grad, weight_grad)
```

```python
import functools

import jax
import jax.numpy as jnp
from jax import lax
from jax.experimental import pallas as pl
from jax.experimental.pallas import tpu as pltpu
from jax.sharding import PartitionSpec as P

K = 31
EPS = 1e-05
HALO = 32
LANES = 128
F32 = jnp.float32
BF16 = jnp.bfloat16
VMEM_LIMIT = 60 * 1024 * 1024


def sigmoid(x):
    return 0.5 * jnp.tanh(0.5 * x) + 0.5


def passed_along(shard, axis, by):
    devices = lax.axis_size(axis)
    pairs = [(i, i + by) for i in range(devices) if 0 <= i + by < devices]
    return lax.ppermute(shard, axis, pairs)


def fir(x_ref, w_ref, lane_block, start, taps, blocks, init):
    accs = [init] * blocks
    weights = [w_ref[lane_block, k] for k in taps]
    for offset in range(K + 8 * (blocks - 1)):
        piece = x_ref[lane_block, pl.ds(start + offset, 8), :]
        for a in range(blocks):
            k = offset - 8 * a
            if 0 <= k < K:
                term = weights[k] * piece
                accs[a] = term if accs[a] is None else accs[a] + term
    return accs


def lane_sums(x):
    return jnp.sum(x.T, axis=0, keepdims=True)


def row_spread(row):
    return jnp.broadcast_to(row, (LANES, LANES)).T


def forward_kernel(
    seq_blocks, values_ref, gates_ref, halo_ref, taps_ref, bias_ref, cot_ref, weight_ref,
    conv_ref, grad_ref, sums_ref, padded,
):
    step = pl.program_id(0)
    rows, chans = values_ref.shape
    lane_blocks = chans // LANES
    chunks = rows // LANES
    depth = cot_ref.shape[1] // chunks
    grad_ref[...] = jnp.zeros_like(grad_ref)

    @pl.when(step % seq_blocks == 0)
    def _():
        for h in range(lane_blocks):
            padded[h, :HALO, :] = halo_ref[0, :, h * LANES : (h + 1) * LANES].astype(F32)

    @pl.when(step % seq_blocks != 0)
    def _():
        for h in range(lane_blocks):
            padded[h, :HALO, :] = padded[h, rows:, :]

    def chunk(i, carry):
        first = pl.multiple_of(i * LANES, LANES)
        here = pl.ds(first, LANES)
        columns = pl.ds(pl.multiple_of(i * depth, depth), depth)
        grad_ref[...] += lax.dot_general(
            cot_ref[:, columns], weight_ref[:, columns], (((1,), (1,)), ((), ())),
            preferred_element_type=F32,
        )
        total = None
        for h in range(lane_blocks):
            lanes = slice(h * LANES, (h + 1) * LANES)
            sig = sigmoid(gates_ref[here, lanes].astype(F32))
            gated = (values_ref[here, lanes].astype(F32) * sig).astype(BF16).astype(F32)
            padded[h, pl.ds(first + HALO, LANES), :] = gated
            for c in range(LANES // 32):
                start = first + c * 32
                accs = fir(padded, taps_ref, h, start + HALO - K + 1, range(K), 4, bias_ref[h])
                for a in range(4):
                    conv_ref[pl.ds(pl.multiple_of(start + 8 * a, 8), 8), lanes] = accs[a]
        total = square = None
        for h in range(lane_blocks):
            conv = conv_ref[here, h * LANES : (h + 1) * LANES]
            total = conv if total is None else total + conv
            square = conv * conv if square is None else square + conv * conv
        row = step * chunks + i
        sums_ref[0, pl.ds(row, 1), :] = lane_sums(total)
        sums_ref[1, pl.ds(row, 1), :] = lane_sums(square)
        return carry

    lax.fori_loop(0, chunks, chunk, 0)


def middle_kernel(
    blocks, total_chans, conv_ref, grad_ref, stats_ref, gain_ref, cot_ref,
    normed_grad_ref, sums_ref, gain_grad_ref, weight_grad_ref, swished,
):
    step = pl.program_id(0)
    rows, chans = conv_ref.shape
    lane_blocks = chans // LANES
    chunks = rows // LANES
    width = cot_ref.shape[1] // chunks
    now = lax.rem(step, 2)
    before = 1 - now

    @pl.when(step == 0)
    def _():
        weight_grad_ref[...] = jnp.zeros_like(weight_grad_ref)
        gain_grad_ref[...] = jnp.zeros_like(gain_grad_ref)
        swished[1] = jnp.zeros(swished.shape[1:], BF16)

    fresh = jnp.where(step < blocks, 1.0, 0.0).astype(F32)
    block = jnp.minimum(step, blocks - 1)

    def chunk(i, carry):
        first = pl.multiple_of(i * LANES, LANES)
        here = pl.ds(first, LANES)
        columns = pl.ds(pl.multiple_of(i * width, width), width)
        weight_grad_ref[:, columns] += jnp.dot(
            swished[before], cot_ref[:, columns], preferred_element_type=F32
        )
        row = block * chunks + i
        mean = stats_ref[0, pl.ds(row, 1), :] / total_chans
        variance = stats_ref[1, pl.ds(row, 1), :] / total_chans - mean * mean
        inverse = row_spread(lax.rsqrt(variance + EPS))
        mean = row_spread(mean)
        plain = weighted = None
        for h in range(lane_blocks):
            lanes = slice(h * LANES, (h + 1) * LANES)
            gain = gain_ref[:, lanes]
            normed = (conv_ref[here, lanes] - mean) * inverse
            scaled = normed * gain
            sig = sigmoid(scaled)
            silu = scaled * sig
            swished[now, lanes, here] = silu.T.astype(BF16)
            scaled_grad = grad_ref[here, lanes] * (sig + silu * (1.0 - sig))
            normed_grad = scaled_grad * gain
            normed_grad_ref[here, lanes] = normed_grad
            product = scaled_grad * normed
            gain_grad_ref[:, lanes] += fresh * jnp.sum(
                product.reshape(LANES // 8, 8, LANES), axis=0
            )
            product = product * gain
            plain = normed_grad if plain is None else plain + normed_grad
            weighted = product if weighted is None else weighted + product
        sums_ref[0, pl.ds(row, 1), :] = lane_sums(plain)
        sums_ref[1, pl.ds(row, 1), :] = lane_sums(weighted)
        return carry

    lax.fori_loop(0, chunks, chunk, 0)


def backward_kernel(
    total_chans, values_ref, gates_ref, halo_ref, next_ref, taps_ref, conv_ref, normed_grad_ref,
    stats_ref, back_ref, gain_grad_ref,
    values_grad_ref, gates_grad_ref, small_ref, padded, wide, taps_acc, bias_acc,
):
    step = pl.program_id(0)
    rows, chans = values_ref.shape
    lane_blocks = chans // LANES
    chunks = rows // LANES

    @pl.when(step == 0)
    def _():
        taps_acc[...] = jnp.zeros_like(taps_acc)
        bias_acc[...] = jnp.zeros_like(bias_acc)

    for h in range(lane_blocks):
        lanes = slice(h * LANES, (h + 1) * LANES)
        padded[h, :HALO, :] = halo_ref[0, :, lanes].astype(F32)
        wide[h, rows:, :] = next_ref[0, :, lanes]

    def prepare(i, carry):
        first = pl.multiple_of(i * LANES, LANES)
        here = pl.ds(first, LANES)
        row = step * chunks + i
        mean = stats_ref[0, pl.ds(row, 1), :] / total_chans
        variance = stats_ref[1, pl.ds(row, 1), :] / total_chans - mean * mean
        inverse = row_spread(lax.rsqrt(variance + EPS))
        mean = row_spread(mean)
        plain = row_spread(back_ref[0, pl.ds(row, 1), :] / total_chans)
        weighted = row_spread(back_ref[1, pl.ds(row, 1), :] / total_chans)
        for h in range(lane_blocks):
            lanes = slice(h * LANES, (h + 1) * LANES)
            sig = sigmoid(gates_ref[here, lanes].astype(F32))
            gated = (values_ref[here, lanes].astype(F32) * sig).astype(BF16).astype(F32)
            padded[h, pl.ds(first + HALO, LANES), :] = gated
            normed = (conv_ref[here, lanes] - mean) * inverse
            conv_grad = inverse * (normed_grad_ref[here, lanes] - plain - normed * weighted)
            wide[h, here, :] = conv_grad
            bias_acc[h] += jnp.sum(conv_grad.reshape(LANES // 8, 8, LANES), axis=0)
        return carry

    lax.fori_loop(0, chunks, prepare, 0)

    for h in range(lane_blocks):

        def correlate(i, accs):
            start = pl.multiple_of(i * 32, 32)
            accs = list(accs)
            grads = [wide[h, pl.ds(pl.multiple_of(start + 8 * a, 8), 8), :] for a in range(4)]
            for offset in range(K + 24):
                piece = padded[h, pl.ds(start + HALO - K + 1 + offset, 8), :]
                for a in range(4):
                    k = offset - 8 * a
                    if 0 <= k < K:
                        accs[k] = accs[k] + grads[a] * piece
            return tuple(accs)

        accs = lax.fori_loop(
            0, rows // 32, correlate, tuple(taps_acc[h, k] for k in range(K))
        )
        for k in range(K):
            taps_acc[h, k] = accs[k]

    def spread(i, carry):
        start = pl.multiple_of(i * 32, 32)
        here = pl.ds(start, 32)
        for h in range(lane_blocks):
            lanes = slice(h * LANES, (h + 1) * LANES)
            accs = fir(wide, taps_ref, h, start, range(K - 1, -1, -1), 4, None)
            gated_grad = jnp.concatenate(accs, axis=0)
            sig = sigmoid(gates_ref[here, lanes].astype(F32))
            values_part = gated_grad * sig
            values_grad_ref[here, lanes] = values_part.astype(BF16)
            gates_grad_ref[here, lanes] = (
                values_part * values_ref[here, lanes].astype(F32) * (1.0 - sig)
            ).astype(BF16)
        return carry

    lax.fori_loop(0, rows // 32, spread, 0)

    @pl.when(step == pl.num_programs(0) - 1)
    def _():
        for h in range(lane_blocks):
            lanes = slice(h * LANES, (h + 1) * LANES)
            for k in range(K):
                small_ref[k : k + 1, lanes] = jnp.sum(taps_acc[h, k], axis=0, keepdims=True)
            small_ref[K : K + 1, lanes] = jnp.sum(bias_acc[h], axis=0, keepdims=True)
            small_ref[K + 1 : K + 2, lanes] = jnp.sum(
                gain_grad_ref[:, lanes], axis=0, keepdims=True
            )
            small_ref[K + 2 :, lanes] = jnp.zeros((small_ref.shape[0] - K - 2, LANES), F32)


def whole(shape):
    return pl.BlockSpec(shape, lambda i: (0,) * len(shape))


def on_device(values_in, gates_in, conv_taps, conv_bias, norm_gain, out_weight, out_grad):
    seqs, tokens, chans = values_in.shape
    width = out_grad.shape[2]
    total_chans = chans * lax.axis_size("tp")
    lane_blocks = chans // LANES
    positions = seqs * tokens
    rows = min(512, tokens)
    blocks = positions // rows
    stat_rows = positions // LANES

    values = values_in.reshape(positions, chans)
    gates = gates_in.reshape(positions, chans)
    cot = out_grad.reshape(positions, width)

    tail_sig = jax.nn.sigmoid(gates_in[:, tokens - HALO :].astype(F32))
    tail = (values_in[:, tokens - HALO :].astype(F32) * tail_sig).astype(BF16)
    before = passed_along(tail, "sp", 1)

    def by_lanes(rows_of):
        count = rows_of.shape[0]
        split = rows_of.astype(F32).reshape(count, lane_blocks, 1, LANES).transpose(1, 0, 2, 3)
        return jnp.broadcast_to(split, (lane_blocks, count, 8, LANES))

    taps8 = by_lanes(conv_taps)
    bias8 = by_lanes(conv_bias[None])[:, 0]
    gain = norm_gain.astype(F32)[None]

    params = pltpu.CompilerParams(
        dimension_semantics=("arbitrary",), vmem_limit_bytes=VMEM_LIMIT
    )
    tile = pl.BlockSpec((rows, chans), lambda i: (i, 0))
    seq_blocks = tokens // rows
    conv, swish_grad, sums = pl.pallas_call(
        functools.partial(forward_kernel, seq_blocks),
        grid=(blocks,),
        in_specs=[
            tile,
            tile,
            pl.BlockSpec((1, HALO, chans), lambda i: (i // seq_blocks, 0, 0)),
            whole(taps8.shape),
            whole(bias8.shape),
            pl.BlockSpec((rows, width), lambda i: (i, 0)),
            whole(out_weight.shape),
        ],
        out_specs=[tile, tile, whole((2, stat_rows, LANES))],
        out_shape=[
            jax.ShapeDtypeStruct((positions, chans), F32),
            jax.ShapeDtypeStruct((positions, chans), F32),
            jax.ShapeDtypeStruct((2, stat_rows, LANES), F32),
        ],
        scratch_shapes=[pltpu.VMEM((lane_blocks, rows + HALO, LANES), F32)],
        compiler_params=params,
        name="forward",
    )(values, gates, before, taps8, bias8, cot, out_weight)
    stats = lax.psum(sums, "tp")

    ahead = pl.BlockSpec((rows, chans), lambda i: (jnp.minimum(i, blocks - 1), 0))
    normed_grad, back, gain_local, weight_local = pl.pallas_call(
        functools.partial(middle_kernel, blocks, total_chans),
        grid=(blocks + 1,),
        in_specs=[
            ahead,
            ahead,
            whole((2, stat_rows, LANES)),
            whole((1, chans)),
            pl.BlockSpec((rows, width), lambda i: (jnp.maximum(i - 1, 0), 0)),
        ],
        out_specs=[
            ahead,
            whole((2, stat_rows, LANES)),
            whole((8, chans)),
            whole((chans, width)),
        ],
        out_shape=[
            jax.ShapeDtypeStruct((positions, chans), F32),
            jax.ShapeDtypeStruct((2, stat_rows, LANES), F32),
            jax.ShapeDtypeStruct((8, chans), F32),
            jax.ShapeDtypeStruct((chans, width), F32),
        ],
        scratch_shapes=[pltpu.VMEM((2, chans, rows), BF16)],
        compiler_params=params,
        name="middle",
    )(conv, swish_grad, stats, gain, cot)
    back = lax.psum(back, "tp")
    weight_grad = lax.psum_scatter(weight_local, "sp", scatter_dimension=0, tiled=True)

    def first_rows(x):
        return x.reshape(seqs, tokens, -1)[:, :HALO]

    def of_rows(x):
        return x.reshape(seqs, tokens, 1)[:, :HALO] / total_chans

    mean = of_rows(stats[0])
    inverse = lax.rsqrt(of_rows(stats[1]) - mean * mean + EPS)
    head = inverse * (
        first_rows(normed_grad)
        - of_rows(back[0])
        - (first_rows(conv) - mean) * inverse * of_rows(back[1])
    )
    after = passed_along(head, "sp", -1)

    seq_tile = pl.BlockSpec((tokens, chans), lambda i: (i, 0))
    halo_tile = pl.BlockSpec((1, HALO, chans), lambda i: (i, 0, 0))
    small_rows = -(-(K + 2) // 8) * 8
    values_grad, gates_grad, small = pl.pallas_call(
        functools.partial(backward_kernel, total_chans),
        grid=(seqs,),
        in_specs=[
            seq_tile,
            seq_tile,
            halo_tile,
            halo_tile,
            whole(taps8.shape),
            seq_tile,
            seq_tile,
            whole((2, stat_rows, LANES)),
            whole((2, stat_rows, LANES)),
            whole((8, chans)),
        ],
        out_specs=[seq_tile, seq_tile, whole((small_rows, chans))],
        out_shape=[
            jax.ShapeDtypeStruct((positions, chans), BF16),
            jax.ShapeDtypeStruct((positions, chans), BF16),
            jax.ShapeDtypeStruct((small_rows, chans), F32),
        ],
        scratch_shapes=[
            pltpu.VMEM((lane_blocks, tokens + HALO, LANES), F32),
            pltpu.VMEM((lane_blocks, tokens + HALO, LANES), F32),
            pltpu.VMEM((lane_blocks, K, 8, LANES), F32),
            pltpu.VMEM((lane_blocks, 8, LANES), F32),
        ],
        compiler_params=params,
        name="backward",
    )(values, gates, before, after, taps8, conv, normed_grad, stats, back, gain_local)
    small = lax.psum(small, "sp")
    return (
        values_grad.reshape(values_in.shape),
        gates_grad.reshape(values_in.shape),
        small[:K],
        small[K + 1],
        small[K],
        weight_grad,
    )


def solution(mesh):
    return jax.shard_map(
        on_device,
        mesh=mesh,
        in_specs=(
            P(None, "sp", "tp"),
            P(None, "sp", "tp"),
            P(None, "tp"),
            P("tp"),
            P("tp"),
            P("tp", None),
            P(None, "sp", None),
        ),
        out_specs=(
            P(None, "sp", "tp"),
            P(None, "sp", "tp"),
            P(None, "tp"),
            P("tp"),
            P("tp"),
            P(("tp", "sp"), None),
        ),
        check_vma=False,
    )
```

```python
import functools

import jax
import jax.numpy as jnp
from jax import lax
from jax.experimental import pallas as pl
from jax.experimental.pallas import tpu as pltpu
from jax.sharding import PartitionSpec as P

K = 31
EPS = 1e-05
HALO = 32
LANES = 128
F32 = jnp.float32
BF16 = jnp.bfloat16
VMEM_LIMIT = 60 * 1024 * 1024


def sigmoid(x):
    return 0.5 * jnp.tanh(0.5 * x) + 0.5


def peer_id(axis, distance):
    devices = lax.axis_size(axis)
    return {axis: lax.rem(lax.axis_index(axis) + distance, devices)}


def greet(pairs):
    barrier = pltpu.get_barrier_semaphore()
    for axis, distance in pairs:
        pl.semaphore_signal(
            barrier, inc=1, device_id=peer_id(axis, distance),
            device_id_type=pl.DeviceIdType.MESH,
        )
    pl.semaphore_wait(barrier, len(pairs))


def remote(src, dst, send_sem, recv_sem, axis, distance):
    return pltpu.make_async_remote_copy(
        src_ref=src, dst_ref=dst, send_sem=send_sem, recv_sem=recv_sem,
        device_id=peer_id(axis, distance), device_id_type=pl.DeviceIdType.MESH,
    )


def fir(x_ref, w_ref, lane_block, start, taps, blocks, init):
    accs = [init] * blocks
    x_block, w_block = lane_block
    weights = [w_ref[w_block, k] for k in taps]
    for offset in range(K + 8 * (blocks - 1)):
        piece = x_ref[x_block, pl.ds(start + offset, 8), :]
        for a in range(blocks):
            k = offset - 8 * a
            if 0 <= k < K:
                term = weights[k] * piece
                accs[a] = term if accs[a] is None else accs[a] + term
    return accs


def lane_sums(x):
    return jnp.sum(x.T, axis=0, keepdims=True)


def row_spread(row):
    return jnp.broadcast_to(row, (LANES, LANES)).T


def forward_kernel(
    seqs, seq_blocks, values_ref, gates_ref, values_before_ref, gates_before_ref, values_hbm,
    gates_hbm, taps_ref, bias_ref, cot_ref, weight_ref,
    conv_ref, grad_ref, sums_ref, halo_ref, padded, values_halo, gates_halo, send_sems, recv_sems,
):
    step = pl.program_id(0)
    rows, chans = values_ref.shape
    lane_blocks = chans // LANES
    chunks = rows // LANES
    depth = cot_ref.shape[1] // chunks
    seq = lax.rem(step, seqs)
    part = seq_blocks - 1 - step // seqs
    block = seq * seq_blocks + part
    sp_devices = lax.axis_size("sp")
    tail = pl.ds(values_hbm.shape[1] - HALO, HALO)
    copies = [
        remote(src.at[:, tail], dst, send_sems.at[n], recv_sems.at[n], "sp", 1)
        for n, (src, dst) in enumerate(((values_hbm, values_halo), (gates_hbm, gates_halo)))
    ]

    @pl.when(step == 0)
    def _():
        greet((("sp", 1), ("sp", sp_devices - 1)))
        for copy in copies:
            copy.start()

    @pl.when(step == seqs * (seq_blocks - 1))
    def _():
        for copy in copies:
            copy.wait()

    grad_ref[...] = jnp.zeros_like(grad_ref)

    def fill(values, gates, keep):
        for h in range(lane_blocks):
            lanes = slice(h * LANES, (h + 1) * LANES)
            sig = sigmoid(gates[:, lanes].astype(F32))
            gated = (values[:, lanes].astype(F32) * sig).astype(BF16).astype(F32)
            padded[h, :HALO, :] = gated * keep

    @pl.when(part == 0)
    def _():
        keep = jnp.where(lax.axis_index("sp") > 0, 1.0, 0.0).astype(F32)
        fill(values_halo[seq], gates_halo[seq], keep)
        for h in range(lane_blocks):
            halo_ref[seq, :, h * LANES : (h + 1) * LANES] = padded[h, :HALO, :]

    @pl.when(part != 0)
    def _():
        fill(values_before_ref[...], gates_before_ref[...], 1.0)

    def chunk(i, carry):
        first = pl.multiple_of(i * LANES, LANES)
        here = pl.ds(first, LANES)
        columns = pl.ds(pl.multiple_of(i * depth, depth), depth)
        grad_ref[...] += lax.dot_general(
            cot_ref[:, columns], weight_ref[:, columns], (((1,), (1,)), ((), ())),
            preferred_element_type=F32,
        )
        total = None
        for h in range(lane_blocks):
            lanes = slice(h * LANES, (h + 1) * LANES)
            sig = sigmoid(gates_ref[here, lanes].astype(F32))
            gated = (values_ref[here, lanes].astype(F32) * sig).astype(BF16).astype(F32)
            padded[h, pl.ds(first + HALO, LANES), :] = gated
            for c in range(LANES // 32):
                start = first + c * 32
                accs = fir(padded, taps_ref, (h, h), start + HALO - K + 1, range(K), 4, bias_ref[h])
                for a in range(4):
                    conv_ref[pl.ds(pl.multiple_of(start + 8 * a, 8), 8), lanes] = accs[a]
        total = square = None
        for h in range(lane_blocks):
            conv = conv_ref[here, h * LANES : (h + 1) * LANES]
            total = conv if total is None else total + conv
            square = conv * conv if square is None else square + conv * conv
        row = block * chunks + i
        sums_ref[0, pl.ds(row, 1), :] = lane_sums(total)
        sums_ref[1, pl.ds(row, 1), :] = lane_sums(square)
        return carry

    lax.fori_loop(0, chunks, chunk, 0)


def middle_kernel(
    blocks, total_chans, conv_ref, grad_ref, own_sums_ref, own_sums_hbm, gain_ref, cot_ref,
    normed_grad_ref, sums_ref, gain_grad_ref, weight_out_ref, stats_ref,
    swished, weight_grad_ref, arrived, send_sems, recv_sems,
):
    step = pl.program_id(0)
    rows, chans = conv_ref.shape
    lane_blocks = chans // LANES
    chunks = rows // LANES
    width = cot_ref.shape[1] // chunks
    now = lax.rem(step, 2)
    before = 1 - now

    @pl.when(step == 0)
    def _():
        peers = range(1, lax.axis_size("tp"))
        greet([("tp", d) for d in peers])
        copies = [
            remote(
                own_sums_hbm, arrived.at[d - 1], send_sems.at[d - 1], recv_sems.at[d - 1], "tp", d
            )
            for d in peers
        ]
        for copy in copies:
            copy.start()
        weight_grad_ref[...] = jnp.zeros_like(weight_grad_ref)
        gain_grad_ref[...] = jnp.zeros_like(gain_grad_ref)
        swished[1] = jnp.zeros(swished.shape[1:], BF16)
        total = own_sums_ref[...]
        for d, copy in zip(peers, copies):
            copy.wait()
            total = total + arrived[d - 1]
        stats_ref[...] = total

    fresh = jnp.where(step < blocks, 1.0, 0.0).astype(F32)
    block = jnp.minimum(step, blocks - 1)

    def chunk(i, carry):
        first = pl.multiple_of(i * LANES, LANES)
        here = pl.ds(first, LANES)
        columns = pl.ds(pl.multiple_of(i * width, width), width)
        weight_grad_ref[:, columns] += jnp.dot(
            swished[before], cot_ref[:, columns], preferred_element_type=F32
        )
        row = block * chunks + i
        mean = stats_ref[0, pl.ds(row, 1), :] / total_chans
        variance = stats_ref[1, pl.ds(row, 1), :] / total_chans - mean * mean
        inverse = row_spread(lax.rsqrt(variance + EPS))
        mean = row_spread(mean)
        plain = weighted = None
        for h in range(lane_blocks):
            lanes = slice(h * LANES, (h + 1) * LANES)
            gain = gain_ref[:, lanes]
            normed = (conv_ref[here, lanes] - mean) * inverse
            scaled = normed * gain
            sig = sigmoid(scaled)
            silu = scaled * sig
            swished[now, lanes, here] = silu.T.astype(BF16)
            scaled_grad = grad_ref[here, lanes] * (sig + silu * (1.0 - sig))
            normed_grad = scaled_grad * gain
            normed_grad_ref[here, lanes] = normed_grad
            product = scaled_grad * normed
            gain_grad_ref[:, lanes] += fresh * jnp.sum(
                product.reshape(LANES // 8, 8, LANES), axis=0
            )
            product = product * gain
            plain = normed_grad if plain is None else plain + normed_grad
            weighted = product if weighted is None else weighted + product
        sums_ref[0, pl.ds(row, 1), :] = lane_sums(plain)
        sums_ref[1, pl.ds(row, 1), :] = lane_sums(weighted)
        return carry

    lax.fori_loop(0, chunks, chunk, 0)

    @pl.when(step == blocks)
    def _():
        weight_out_ref[...] = weight_grad_ref[...].astype(BF16)


def backward_kernel(
    total_chans, seqs, values_hbm, gates_hbm, conv_hbm, normed_grad_hbm, weight_hbm, back_hbm,
    halo_ref, taps_ref, stats_ref, own_back_ref, gain_grad_ref,
    values_grad_hbm, gates_grad_hbm, small_ref, weight_grad_ref,
    values, gates, conv, normed_grad, padded, wide, heads, back, back_arrived, small,
    small_arrived, own_weight, weight_arrived, local_sems, out_sems, weight_sem,
    back_send, back_recv, weight_send, weight_recv, head_send, head_recv, small_send, small_recv,
):
    positions, chans = values.shape
    tokens = positions // seqs
    lane_blocks = chans // LANES
    chunks = tokens // LANES
    sp_devices = lax.axis_size("sp")
    me = lax.axis_index("sp")
    tp_peers = range(1, lax.axis_size("tp"))
    sp_peers = range(1, sp_devices)

    def rows_of(s):
        return pl.ds(s * tokens, tokens)

    loads = []
    for s in range(seqs):
        pairs = ((values_hbm, values), (gates_hbm, gates), (conv_hbm, conv),
                 (normed_grad_hbm, normed_grad))
        loads.append([
            pltpu.make_async_copy(src.at[rows_of(s)], dst.at[rows_of(s)], local_sems.at[s, n])
            for n, (src, dst) in enumerate(pairs)
        ])
        for copy in loads[s]:
            copy.start()
    greet([("tp", d) for d in tp_peers] + [("sp", d) for d in sp_peers])
    back_copies = [
        remote(back_hbm, back_arrived.at[d - 1], back_send.at[d - 1], back_recv.at[d - 1], "tp", d)
        for d in tp_peers
    ]
    for copy in back_copies:
        copy.start()
    weight_copies = [
        remote(
            weight_hbm.at[lax.rem(me + d, sp_devices)], weight_arrived.at[d - 1],
            weight_send.at[d - 1], weight_recv.at[d - 1], "sp", d,
        )
        for d in sp_peers
    ]
    for copy in weight_copies:
        copy.start()
    own_copy = pltpu.make_async_copy(weight_hbm.at[me], own_weight, weight_sem)
    own_copy.start()

    total = own_back_ref[...]
    for d, copy in zip(tp_peers, back_copies):
        copy.wait()
        total = total + back_arrived[d - 1]
    back[...] = total

    for s in range(seqs):
        for h in range(lane_blocks):
            padded[s * lane_blocks + h, :HALO, :] = halo_ref[s, :, h * LANES : (h + 1) * LANES]
    bias_accs = tuple(jnp.zeros((8, LANES), F32) for _ in range(lane_blocks))
    for s in range(seqs):
        for copy in loads[s]:
            copy.wait()

        def prepare(i, accs):
            accs = list(accs)
            first = pl.multiple_of(i * LANES, LANES)
            here = pl.ds(s * tokens + first, LANES)
            row = s * chunks + i
            mean = stats_ref[0, pl.ds(row, 1), :] / total_chans
            variance = stats_ref[1, pl.ds(row, 1), :] / total_chans - mean * mean
            inverse = row_spread(lax.rsqrt(variance + EPS))
            mean = row_spread(mean)
            plain = row_spread(back[0, pl.ds(row, 1), :] / total_chans)
            weighted = row_spread(back[1, pl.ds(row, 1), :] / total_chans)
            for h in range(lane_blocks):
                lanes = slice(h * LANES, (h + 1) * LANES)
                sig = sigmoid(gates[here, lanes].astype(F32))
                gated = (values[here, lanes].astype(F32) * sig).astype(BF16).astype(F32)
                padded[s * lane_blocks + h, pl.ds(first + HALO, LANES), :] = gated
                normed = (conv[here, lanes] - mean) * inverse
                conv_grad = inverse * (normed_grad[here, lanes] - plain - normed * weighted)
                wide[s * lane_blocks + h, pl.ds(first, LANES), :] = conv_grad
                accs[h] = accs[h] + jnp.sum(conv_grad.reshape(LANES // 8, 8, LANES), axis=0)
            return tuple(accs)

        bias_accs = lax.fori_loop(0, chunks, prepare, bias_accs)

    head_copy = remote(
        wide.at[:, pl.ds(0, HALO)], heads, head_send, head_recv, "sp", sp_devices - 1
    )
    head_copy.start()

    for h in range(lane_blocks):
        accs = tuple(jnp.zeros((8, LANES), F32) for _ in range(K))
        for s in range(seqs):
            where = s * lane_blocks + h

            def correlate(i, accs):
                start = pl.multiple_of(i * 32, 32)
                accs = list(accs)
                grads = [
                    wide[where, pl.ds(pl.multiple_of(start + 8 * a, 8), 8), :] for a in range(4)
                ]
                for offset in range(K + 24):
                    piece = padded[where, pl.ds(start + HALO - K + 1 + offset, 8), :]
                    for a in range(4):
                        k = offset - 8 * a
                        if 0 <= k < K:
                            accs[k] = accs[k] + grads[a] * piece
                return tuple(accs)

            accs = lax.fori_loop(0, tokens // 32, correlate, accs)
        lanes = slice(h * LANES, (h + 1) * LANES)
        for k in range(K):
            small[k : k + 1, lanes] = jnp.sum(accs[k], axis=0, keepdims=True)
        small[K : K + 1, lanes] = jnp.sum(bias_accs[h], axis=0, keepdims=True)
        small[K + 1 : K + 2, lanes] = jnp.sum(gain_grad_ref[:, lanes], axis=0, keepdims=True)
        small[K + 2 :, lanes] = jnp.zeros((small.shape[0] - K - 2, LANES), F32)

    small_copies = [
        remote(small, small_arrived.at[d - 1], small_send.at[d - 1], small_recv.at[d - 1], "sp", d)
        for d in sp_peers
    ]

    def spread_chunk(s, start):
        here = pl.ds(pl.multiple_of(s * tokens + start, 32), 32)
        for h in range(lane_blocks):
            lanes = slice(h * LANES, (h + 1) * LANES)
            accs = fir(
                wide, taps_ref, (s * lane_blocks + h, h), start, range(K - 1, -1, -1), 4, None
            )
            gated_grad = jnp.concatenate(accs, axis=0)
            sig = sigmoid(gates[here, lanes].astype(F32))
            values_part = gated_grad * sig
            gates_part = values_part * values[here, lanes].astype(F32) * (1.0 - sig)
            values[here, lanes] = values_part.astype(BF16)
            gates[here, lanes] = gates_part.astype(BF16)

    for s in range(seqs):

        def spread(i, carry):
            spread_chunk(s, pl.multiple_of(i * 32, 32))
            return carry

        lax.fori_loop(0, tokens // 32 - 1, spread, 0)
        if s == 0:
            for copy in small_copies:
                copy.start()

    head_copy.wait()
    keep = jnp.where(me < sp_devices - 1, 1.0, 0.0).astype(F32)
    stores = []
    for s in range(seqs):
        for h in range(lane_blocks):
            where = s * lane_blocks + h
            wide[where, tokens:, :] = heads[where] * keep
        spread_chunk(s, tokens - 32)
        for n, (src, dst) in enumerate(((values, values_grad_hbm), (gates, gates_grad_hbm))):
            copy = pltpu.make_async_copy(
                src.at[rows_of(s)], dst.at[rows_of(s)], out_sems.at[s, n]
            )
            copy.start()
            stores.append(copy)

    own_copy.wait()
    weight_grad_ref[...] = own_weight[...].astype(F32)
    for d, copy in zip(sp_peers, weight_copies):
        copy.wait()
        weight_grad_ref[...] += weight_arrived[d - 1].astype(F32)
    sum_small = small[...]
    for d, copy in zip(sp_peers, small_copies):
        copy.wait()
        sum_small = sum_small + small_arrived[d - 1]
    small_ref[...] = sum_small
    for copy in stores:
        copy.wait()


def whole(shape):
    return pl.BlockSpec(shape, lambda i: (0,) * len(shape))


def on_device(values_in, gates_in, conv_taps, conv_bias, norm_gain, out_weight, out_grad):
    seqs, tokens, chans = values_in.shape
    width = out_grad.shape[2]
    total_chans = chans * lax.axis_size("tp")
    lane_blocks = chans // LANES
    positions = seqs * tokens
    rows = min(512, tokens)
    blocks = positions // rows
    stat_rows = positions // LANES

    values = values_in.reshape(positions, chans)
    gates = gates_in.reshape(positions, chans)
    cot = out_grad.reshape(positions, width)

    def by_lanes(rows_of):
        count = rows_of.shape[0]
        split = rows_of.astype(F32).reshape(count, lane_blocks, 1, LANES).transpose(1, 0, 2, 3)
        return jnp.broadcast_to(split, (lane_blocks, count, 8, LANES))

    taps8 = by_lanes(conv_taps)
    bias8 = by_lanes(conv_bias[None])[:, 0]
    gain = norm_gain.astype(F32)[None]

    tp_others = lax.axis_size("tp") - 1
    sp_devices = lax.axis_size("sp")
    sp_others = sp_devices - 1

    def params(ident):
        return pltpu.CompilerParams(
            dimension_semantics=("arbitrary",), vmem_limit_bytes=VMEM_LIMIT,
            collective_id=ident, has_side_effects=True,
        )

    def dma(*shape):
        return pltpu.SemaphoreType.DMA(shape)

    anywhere = pl.BlockSpec(memory_space=pl.ANY)
    stats_shape = (2, stat_rows, LANES)
    seq_blocks = tokens // rows

    def block_of(i):
        return i % seqs * seq_blocks + seq_blocks - 1 - i // seqs

    tile = pl.BlockSpec((rows, chans), lambda i: (block_of(i), 0))
    ahead_halo = pl.BlockSpec(
        (HALO, chans), lambda i: (jnp.maximum(block_of(i) * (rows // HALO) - 1, 0), 0)
    )
    conv, swish_grad, sums, halo = pl.pallas_call(
        functools.partial(forward_kernel, seqs, seq_blocks),
        grid=(blocks,),
        in_specs=[
            tile, tile, ahead_halo, ahead_halo, anywhere, anywhere,
            whole(taps8.shape),
            whole(bias8.shape),
            pl.BlockSpec((rows, width), lambda i: (block_of(i), 0)),
            whole(out_weight.shape),
        ],
        out_specs=[tile, tile, whole(stats_shape), whole((seqs, HALO, chans))],
        out_shape=[
            jax.ShapeDtypeStruct((positions, chans), F32),
            jax.ShapeDtypeStruct((positions, chans), F32),
            jax.ShapeDtypeStruct(stats_shape, F32),
            jax.ShapeDtypeStruct((seqs, HALO, chans), F32),
        ],
        scratch_shapes=[
            pltpu.VMEM((lane_blocks, rows + HALO, LANES), F32),
            pltpu.VMEM((seqs, HALO, chans), BF16),
            pltpu.VMEM((seqs, HALO, chans), BF16),
            dma(2),
            dma(2),
        ],
        compiler_params=params(0),
        name="forward",
    )(values, gates, values, gates, values_in, gates_in, taps8, bias8, cot, out_weight)

    ahead = pl.BlockSpec((rows, chans), lambda i: (jnp.minimum(i, blocks - 1), 0))
    normed_grad, back, gain_local, weight_local, stats = pl.pallas_call(
        functools.partial(middle_kernel, blocks, total_chans),
        grid=(blocks + 1,),
        in_specs=[
            ahead,
            ahead,
            whole(stats_shape),
            anywhere,
            whole((1, chans)),
            pl.BlockSpec((rows, width), lambda i: (jnp.maximum(i - 1, 0), 0)),
        ],
        out_specs=[
            ahead,
            whole(stats_shape),
            whole((8, chans)),
            whole((chans, width)),
            whole(stats_shape),
        ],
        out_shape=[
            jax.ShapeDtypeStruct((positions, chans), F32),
            jax.ShapeDtypeStruct(stats_shape, F32),
            jax.ShapeDtypeStruct((8, chans), F32),
            jax.ShapeDtypeStruct((chans, width), BF16),
            jax.ShapeDtypeStruct(stats_shape, F32),
        ],
        scratch_shapes=[
            pltpu.VMEM((2, chans, rows), BF16),
            pltpu.VMEM((chans, width), F32),
            pltpu.VMEM((tp_others, *stats_shape), F32),
            dma(tp_others),
            dma(tp_others),
        ],
        compiler_params=params(1),
        name="middle",
    )(conv, swish_grad, sums, sums, gain, cot)

    small_rows = -(-(K + 2) // 8) * 8
    weight_rows = chans // sp_devices
    padded_shape = (seqs * lane_blocks, tokens + HALO, LANES)
    values_grad, gates_grad, small, weight_grad = pl.pallas_call(
        functools.partial(backward_kernel, total_chans, seqs),
        in_specs=[anywhere] * 6 + [pl.BlockSpec(memory_space=pltpu.VMEM)] * 5,
        out_specs=[anywhere] * 2 + [pl.BlockSpec(memory_space=pltpu.VMEM)] * 2,
        out_shape=[
            jax.ShapeDtypeStruct((positions, chans), BF16),
            jax.ShapeDtypeStruct((positions, chans), BF16),
            jax.ShapeDtypeStruct((small_rows, chans), F32),
            jax.ShapeDtypeStruct((weight_rows, width), F32),
        ],
        scratch_shapes=[
            pltpu.VMEM((positions, chans), BF16),
            pltpu.VMEM((positions, chans), BF16),
            pltpu.VMEM((positions, chans), F32),
            pltpu.VMEM((positions, chans), F32),
            pltpu.VMEM(padded_shape, F32),
            pltpu.VMEM(padded_shape, F32),
            pltpu.VMEM((seqs * lane_blocks, HALO, LANES), F32),
            pltpu.VMEM(stats_shape, F32),
            pltpu.VMEM((tp_others, *stats_shape), F32),
            pltpu.VMEM((small_rows, chans), F32),
            pltpu.VMEM((sp_others, small_rows, chans), F32),
            pltpu.VMEM((weight_rows, width), BF16),
            pltpu.VMEM((sp_others, weight_rows, width), BF16),
            dma(seqs, 4),
            dma(seqs, 2),
            pltpu.SemaphoreType.DMA,
            dma(tp_others),
            dma(tp_others),
            dma(sp_others),
            dma(sp_others),
            pltpu.SemaphoreType.DMA,
            pltpu.SemaphoreType.DMA,
            dma(sp_others),
            dma(sp_others),
        ],
        compiler_params=pltpu.CompilerParams(
            vmem_limit_bytes=VMEM_LIMIT, collective_id=2, has_side_effects=True
        ),
        name="backward",
    )(
        values, gates, conv, normed_grad,
        weight_local.reshape(sp_devices, weight_rows, width), back,
        halo, taps8, stats, back, gain_local,
    )
    return (
        values_grad.reshape(values_in.shape),
        gates_grad.reshape(values_in.shape),
        small[:K],
        small[K + 1],
        small[K],
        weight_grad,
    )


def solution(mesh):
    return jax.shard_map(
        on_device,
        mesh=mesh,
        in_specs=(
            P(None, "sp", "tp"),
            P(None, "sp", "tp"),
            P(None, "tp"),
            P("tp"),
            P("tp"),
            P("tp", None),
            P(None, "sp", None),
        ),
        out_specs=(
            P(None, "sp", "tp"),
            P(None, "sp", "tp"),
            P(None, "tp"),
            P("tp"),
            P("tp"),
            P(("tp", "sp"), None),
        ),
        check_vma=False,
    )
```

```python
import functools

import jax
import jax.numpy as jnp
from jax import lax
from jax.experimental import pallas as pl
from jax.experimental.pallas import tpu as pltpu
from jax.sharding import PartitionSpec as P

K = 31
EPS = 1e-05
HALO = 32
PAIR = 2
LANES = 128
F32 = jnp.float32
BF16 = jnp.bfloat16
VMEM_LIMIT = 60 * 1024 * 1024


def sigmoid(x):
    return 0.5 * jnp.tanh(0.5 * x) + 0.5


def peer_id(axis, distance):
    devices = lax.axis_size(axis)
    return {axis: lax.rem(lax.axis_index(axis) + distance, devices)}


def greet(pairs):
    barrier = pltpu.get_barrier_semaphore()
    for axis, distance in pairs:
        pl.semaphore_signal(
            barrier, inc=1, device_id=peer_id(axis, distance),
            device_id_type=pl.DeviceIdType.MESH,
        )
    pl.semaphore_wait(barrier, len(pairs))


def remote(src, dst, send_sem, recv_sem, axis, distance):
    return pltpu.make_async_remote_copy(
        src_ref=src, dst_ref=dst, send_sem=send_sem, recv_sem=recv_sem,
        device_id=peer_id(axis, distance), device_id_type=pl.DeviceIdType.MESH,
    )


def fir(x_ref, w_ref, lane_block, start, taps, blocks, init):
    accs = [init] * blocks
    x_block, w_block = lane_block
    weights = [w_ref[w_block, k] for k in taps]
    for offset in range(K + 8 * (blocks - 1)):
        piece = x_ref[x_block, pl.ds(start + offset, 8), :]
        for a in range(blocks):
            k = offset - 8 * a
            if 0 <= k < K:
                term = weights[k] * piece
                accs[a] = term if accs[a] is None else accs[a] + term
    return accs


def lane_sums(x):
    return jnp.sum(x.T, axis=0, keepdims=True)


def row_spread(row):
    return jnp.broadcast_to(row, (LANES, LANES)).T


def forward_kernel(
    seqs, seq_blocks, values_ref, gates_ref, values_before_ref, gates_before_ref, values_hbm,
    gates_hbm, raw_taps_ref, bias_ref, cot_ref, weight_ref,
    conv_ref, grad_ref, sums_ref, halo_ref, taps_ref, padded, values_halo, gates_halo, send_sems, recv_sems,
):
    step = pl.program_id(0)
    rows, chans = values_ref.shape
    lane_blocks = chans // LANES
    chunks = rows // LANES
    depth = cot_ref.shape[1] // chunks
    seq = lax.rem(step, seqs)
    part = seq_blocks - 1 - step // seqs
    block = seq * seq_blocks + part
    sp_devices = lax.axis_size("sp")
    tail = pl.ds(values_hbm.shape[1] - HALO, HALO)
    copies = [
        remote(src.at[:, tail], dst, send_sems.at[n], recv_sems.at[n], "sp", 1)
        for n, (src, dst) in enumerate(((values_hbm, values_halo), (gates_hbm, gates_halo)))
    ]

    @pl.when(step == 0)
    def _():
        greet((("sp", 1), ("sp", sp_devices - 1)))
        for copy in copies:
            copy.start()
        rows_of_taps = raw_taps_ref[...].astype(F32)
        for h in range(lane_blocks):
            for k in range(K):
                taps_ref[h, k] = jnp.broadcast_to(
                    rows_of_taps[k : k + 1, h * LANES : (h + 1) * LANES], (8, LANES)
                )

    @pl.when(step == seqs * (seq_blocks - 1))
    def _():
        for copy in copies:
            copy.wait()

    grad_ref[...] = jnp.zeros_like(grad_ref)

    def fill(values, gates, keep):
        for h in range(lane_blocks):
            lanes = slice(h * LANES, (h + 1) * LANES)
            sig = sigmoid(gates[:, lanes].astype(F32))
            gated = (values[:, lanes].astype(F32) * sig).astype(BF16).astype(F32)
            padded[h, :HALO, :] = gated * keep

    @pl.when(part == 0)
    def _():
        keep = jnp.where(lax.axis_index("sp") > 0, 1.0, 0.0).astype(F32)
        fill(values_halo[seq], gates_halo[seq], keep)
        for h in range(lane_blocks):
            halo_ref[seq, :, h * LANES : (h + 1) * LANES] = padded[h, :HALO, :]

    @pl.when(part != 0)
    def _():
        fill(values_before_ref[...], gates_before_ref[...], 1.0)

    def chunk(i, carry):
        first = pl.multiple_of(i * LANES, LANES)
        here = pl.ds(first, LANES)
        columns = pl.ds(pl.multiple_of(i * depth, depth), depth)
        grad_ref[...] += lax.dot_general(
            cot_ref[:, columns], weight_ref[:, columns], (((1,), (1,)), ((), ())),
            preferred_element_type=F32,
        )
        total = None
        for h in range(lane_blocks):
            lanes = slice(h * LANES, (h + 1) * LANES)
            sig = sigmoid(gates_ref[here, lanes].astype(F32))
            gated = (values_ref[here, lanes].astype(F32) * sig).astype(BF16).astype(F32)
            padded[h, pl.ds(first + HALO, LANES), :] = gated
            bias = jnp.broadcast_to(bias_ref[:, lanes].astype(F32), (8, LANES))
            for c in range(LANES // 32):
                start = first + c * 32
                accs = fir(padded, taps_ref, (h, h), start + HALO - K + 1, range(K), 4, bias)
                for a in range(4):
                    conv_ref[pl.ds(pl.multiple_of(start + 8 * a, 8), 8), lanes] = accs[a]
        total = square = None
        for h in range(lane_blocks):
            conv = conv_ref[here, h * LANES : (h + 1) * LANES]
            total = conv if total is None else total + conv
            square = conv * conv if square is None else square + conv * conv
        row = block * chunks + i
        sums_ref[0, pl.ds(row, 1), :] = lane_sums(total)
        sums_ref[1, pl.ds(row, 1), :] = lane_sums(square)
        return carry

    lax.fori_loop(0, chunks, chunk, 0)


def middle_kernel(
    blocks, total_chans, conv_ref, grad_ref, own_sums_ref, own_sums_hbm, gain_ref, cot_ref,
    normed_grad_ref, sums_ref, gain_grad_ref, weight_out_ref, stats_ref,
    swished, weight_grad_ref, arrived, send_sems, recv_sems,
):
    step = pl.program_id(0)
    rows, chans = conv_ref.shape
    lane_blocks = chans // LANES
    chunks = rows // LANES
    width = cot_ref.shape[1] // chunks
    now = lax.rem(step, 2)
    before = 1 - now

    @pl.when(step == 0)
    def _():
        peers = range(1, lax.axis_size("tp"))
        greet([("tp", d) for d in peers])
        copies = [
            remote(
                own_sums_hbm, arrived.at[d - 1], send_sems.at[d - 1], recv_sems.at[d - 1], "tp", d
            )
            for d in peers
        ]
        for copy in copies:
            copy.start()
        weight_grad_ref[...] = jnp.zeros_like(weight_grad_ref)
        gain_grad_ref[...] = jnp.zeros_like(gain_grad_ref)
        swished[1] = jnp.zeros(swished.shape[1:], BF16)
        total = own_sums_ref[...]
        for d, copy in zip(peers, copies):
            copy.wait()
            total = total + arrived[d - 1]
        stats_ref[...] = total

    fresh = jnp.where(step < blocks, 1.0, 0.0).astype(F32)
    block = jnp.minimum(step, blocks - 1)

    def chunk(i, carry):
        first = pl.multiple_of(i * LANES, LANES)
        here = pl.ds(first, LANES)
        columns = pl.ds(pl.multiple_of(i * width, width), width)
        weight_grad_ref[:, columns] += jnp.dot(
            swished[before], cot_ref[:, columns], preferred_element_type=F32
        )
        row = block * chunks + i
        mean = stats_ref[0, pl.ds(row, 1), :] / total_chans
        variance = stats_ref[1, pl.ds(row, 1), :] / total_chans - mean * mean
        inverse = row_spread(lax.rsqrt(variance + EPS))
        mean = row_spread(mean)
        plain = weighted = None
        for h in range(lane_blocks):
            lanes = slice(h * LANES, (h + 1) * LANES)
            gain = gain_ref[:, lanes]
            normed = (conv_ref[here, lanes] - mean) * inverse
            scaled = normed * gain
            sig = sigmoid(scaled)
            silu = scaled * sig
            swished[now, lanes, here] = silu.T.astype(BF16)
            scaled_grad = grad_ref[here, lanes] * (sig + silu * (1.0 - sig))
            normed_grad = scaled_grad * gain
            normed_grad_ref[here, lanes] = normed_grad
            product = scaled_grad * normed
            gain_grad_ref[:, lanes] += fresh * jnp.sum(
                product.reshape(LANES // 8, 8, LANES), axis=0
            )
            product = product * gain
            plain = normed_grad if plain is None else plain + normed_grad
            weighted = product if weighted is None else weighted + product
        sums_ref[0, pl.ds(row, 1), :] = lane_sums(plain)
        sums_ref[1, pl.ds(row, 1), :] = lane_sums(weighted)
        return carry

    lax.fori_loop(0, chunks, chunk, 0)

    @pl.when(step == blocks)
    def _():
        weight_out_ref[...] = weight_grad_ref[...].astype(BF16)


def backward_kernel(
    total_chans, seqs, values_hbm, gates_hbm, conv_hbm, normed_grad_hbm, weight_hbm, back_hbm,
    halo_ref, taps_ref, stats_ref, own_back_ref, gain_grad_ref,
    values_grad_hbm, gates_grad_hbm, small_ref, weight_grad_ref,
    values, gates, conv, normed_grad, padded, wide, heads, back, back_arrived, small,
    small_arrived, own_weight, pair_arrived, weight_arrived, local_sems, out_sems, weight_sem,
    pair_send, pair_recv,
    back_send, back_recv, weight_send, weight_recv, head_send, head_recv, small_send, small_recv,
):
    positions, chans = values.shape
    tokens = positions // seqs
    lane_blocks = chans // LANES
    chunks = tokens // LANES
    sp_devices = lax.axis_size("sp")
    me = lax.axis_index("sp")
    tp_peers = range(1, lax.axis_size("tp"))
    sp_peers = range(1, sp_devices)

    def rows_of(s):
        return pl.ds(s * tokens, tokens)

    loads = []
    for s in range(seqs):
        pairs = ((values_hbm, values), (gates_hbm, gates), (conv_hbm, conv),
                 (normed_grad_hbm, normed_grad))
        loads.append([
            pltpu.make_async_copy(src.at[rows_of(s)], dst.at[rows_of(s)], local_sems.at[s, n])
            for n, (src, dst) in enumerate(pairs)
        ])
        for copy in loads[s]:
            copy.start()
    greet([("tp", d) for d in tp_peers] + [("sp", d) for d in sp_peers])
    back_copies = [
        remote(back_hbm, back_arrived.at[d - 1], back_send.at[d - 1], back_recv.at[d - 1], "tp", d)
        for d in tp_peers
    ]
    for copy in back_copies:
        copy.start()
    group = PAIR if sp_devices % PAIR == 0 else 1
    groups = sp_devices // group
    inner = lax.rem(me, group)
    outer = me // group
    order = list(range(1, groups)) + [0]
    pair_copies, own_copies, weight_copies = {}, {}, {}
    for d in order:
        base = lax.rem(outer + d, groups) * group
        own_copies[d] = pltpu.make_async_copy(
            weight_hbm.at[base + inner], own_weight.at[d], weight_sem.at[d]
        )
        own_copies[d].start()
        if group > 1:
            pair_copies[d] = remote(
                weight_hbm.at[base + 1 - inner], pair_arrived.at[d], pair_send.at[d],
                pair_recv.at[d], "sp", sp_devices + 1 - 2 * inner,
            )
            pair_copies[d].start()
        if d > 0:
            weight_copies[d] = remote(
                own_weight.at[d], weight_arrived.at[d - 1], weight_send.at[d - 1],
                weight_recv.at[d - 1], "sp", d * group,
            )

    def pair_sum(d):
        own_copies[d].wait()
        total = own_weight[d].astype(F32)
        if group > 1:
            pair_copies[d].wait()
            total = total + pair_arrived[d].astype(F32)
        return total

    slots = seqs * lane_blocks + seqs
    todo = {}
    for n, d in enumerate(order[:-1]):
        at = min(1 + n * slots // groups, slots - 2)
        todo.setdefault(at, []).append((True, d))
        todo.setdefault(at + 1, []).append((False, d))
    slot = [0]

    def forward_slices():
        for adds, d in todo.pop(slot[0], []):
            if adds:
                own_weight[d] = pair_sum(d).astype(BF16)
            else:
                weight_copies[d].start()
        slot[0] += 1

    total = own_back_ref[...]
    for d, copy in zip(tp_peers, back_copies):
        copy.wait()
        total = total + back_arrived[d - 1]
    back[...] = total

    for s in range(seqs):
        for h in range(lane_blocks):
            padded[s * lane_blocks + h, :HALO, :] = halo_ref[s, :, h * LANES : (h + 1) * LANES]
    bias_accs = tuple(jnp.zeros((8, LANES), F32) for _ in range(lane_blocks))
    for s in range(seqs):
        for copy in loads[s]:
            copy.wait()

        def prepare(i, accs):
            accs = list(accs)
            first = pl.multiple_of(i * LANES, LANES)
            here = pl.ds(s * tokens + first, LANES)
            row = s * chunks + i
            mean = stats_ref[0, pl.ds(row, 1), :] / total_chans
            variance = stats_ref[1, pl.ds(row, 1), :] / total_chans - mean * mean
            inverse = row_spread(lax.rsqrt(variance + EPS))
            mean = row_spread(mean)
            plain = row_spread(back[0, pl.ds(row, 1), :] / total_chans)
            weighted = row_spread(back[1, pl.ds(row, 1), :] / total_chans)
            for h in range(lane_blocks):
                lanes = slice(h * LANES, (h + 1) * LANES)
                sig = sigmoid(gates[here, lanes].astype(F32))
                gated = (values[here, lanes].astype(F32) * sig).astype(BF16).astype(F32)
                padded[s * lane_blocks + h, pl.ds(first + HALO, LANES), :] = gated
                normed = (conv[here, lanes] - mean) * inverse
                conv_grad = inverse * (normed_grad[here, lanes] - plain - normed * weighted)
                wide[s * lane_blocks + h, pl.ds(first, LANES), :] = conv_grad
                accs[h] = accs[h] + jnp.sum(conv_grad.reshape(LANES // 8, 8, LANES), axis=0)
            return tuple(accs)

        bias_accs = lax.fori_loop(0, chunks, prepare, bias_accs)

    head_copy = remote(
        wide.at[:, pl.ds(0, HALO)], heads, head_send, head_recv, "sp", sp_devices - 1
    )
    head_copy.start()

    for h in range(lane_blocks):
        accs = tuple(jnp.zeros((8, LANES), F32) for _ in range(K))
        for s in range(seqs):
            where = s * lane_blocks + h

            def correlate(i, accs):
                start = pl.multiple_of(i * 32, 32)
                accs = list(accs)
                grads = [
                    wide[where, pl.ds(pl.multiple_of(start + 8 * a, 8), 8), :] for a in range(4)
                ]
                for offset in range(K + 24):
                    piece = padded[where, pl.ds(start + HALO - K + 1 + offset, 8), :]
                    for a in range(4):
                        k = offset - 8 * a
                        if 0 <= k < K:
                            accs[k] = accs[k] + grads[a] * piece
                return tuple(accs)

            accs = lax.fori_loop(0, tokens // 32, correlate, accs)
            forward_slices()
        lanes = slice(h * LANES, (h + 1) * LANES)
        for k in range(K):
            small[k : k + 1, lanes] = jnp.sum(accs[k], axis=0, keepdims=True)
        small[K : K + 1, lanes] = jnp.sum(bias_accs[h], axis=0, keepdims=True)
        small[K + 1 : K + 2, lanes] = jnp.sum(gain_grad_ref[:, lanes], axis=0, keepdims=True)
        small[K + 2 :, lanes] = jnp.zeros((small.shape[0] - K - 2, LANES), F32)

    small_copies = [
        remote(small, small_arrived.at[d - 1], small_send.at[d - 1], small_recv.at[d - 1], "sp", d)
        for d in sp_peers
    ]

    def spread_chunk(s, start):
        here = pl.ds(pl.multiple_of(s * tokens + start, 32), 32)
        for h in range(lane_blocks):
            lanes = slice(h * LANES, (h + 1) * LANES)
            accs = fir(
                wide, taps_ref, (s * lane_blocks + h, h), start, range(K - 1, -1, -1), 4, None
            )
            gated_grad = jnp.concatenate(accs, axis=0)
            sig = sigmoid(gates[here, lanes].astype(F32))
            values_part = gated_grad * sig
            gates_part = values_part * values[here, lanes].astype(F32) * (1.0 - sig)
            values[here, lanes] = values_part.astype(BF16)
            gates[here, lanes] = gates_part.astype(BF16)

    for s in range(seqs):

        def spread(i, carry):
            spread_chunk(s, pl.multiple_of(i * 32, 32))
            return carry

        lax.fori_loop(0, tokens // 32 - 1, spread, 0)
        forward_slices()
        if s == 0:
            for copy in small_copies:
                copy.start()

    while todo:
        forward_slices()
    head_copy.wait()
    keep = jnp.where(me < sp_devices - 1, 1.0, 0.0).astype(F32)
    stores = []
    for s in range(seqs):
        for h in range(lane_blocks):
            where = s * lane_blocks + h
            wide[where, tokens:, :] = heads[where] * keep
        spread_chunk(s, tokens - 32)
        for n, (src, dst) in enumerate(((values, values_grad_hbm), (gates, gates_grad_hbm))):
            copy = pltpu.make_async_copy(
                src.at[rows_of(s)], dst.at[rows_of(s)], out_sems.at[s, n]
            )
            copy.start()
            stores.append(copy)

    weight_grad_ref[...] = pair_sum(0)
    for d, copy in weight_copies.items():
        copy.wait()
        weight_grad_ref[...] += weight_arrived[d - 1].astype(F32)
    sum_small = small[...]
    for d, copy in zip(sp_peers, small_copies):
        copy.wait()
        sum_small = sum_small + small_arrived[d - 1]
    small_ref[...] = sum_small
    for copy in stores:
        copy.wait()


def whole(shape):
    return pl.BlockSpec(shape, lambda i: (0,) * len(shape))


def on_device(values_in, gates_in, conv_taps, conv_bias, norm_gain, out_weight, out_grad):
    seqs, tokens, chans = values_in.shape
    width = out_grad.shape[2]
    total_chans = chans * lax.axis_size("tp")
    lane_blocks = chans // LANES
    positions = seqs * tokens
    rows = min(512, tokens)
    blocks = positions // rows
    stat_rows = positions // LANES

    values = values_in.reshape(positions, chans)
    gates = gates_in.reshape(positions, chans)
    cot = out_grad.reshape(positions, width)

    gain = norm_gain.astype(F32)[None]

    tp_others = lax.axis_size("tp") - 1
    sp_devices = lax.axis_size("sp")
    sp_others = sp_devices - 1

    def params(ident):
        return pltpu.CompilerParams(
            dimension_semantics=("arbitrary",), vmem_limit_bytes=VMEM_LIMIT,
            collective_id=ident, has_side_effects=True,
        )

    def dma(*shape):
        return pltpu.SemaphoreType.DMA(shape)

    anywhere = pl.BlockSpec(memory_space=pl.ANY)
    stats_shape = (2, stat_rows, LANES)
    taps_shape = (lane_blocks, K, 8, LANES)
    seq_blocks = tokens // rows

    def block_of(i):
        return i % seqs * seq_blocks + seq_blocks - 1 - i // seqs

    tile = pl.BlockSpec((rows, chans), lambda i: (block_of(i), 0))
    ahead_halo = pl.BlockSpec(
        (HALO, chans), lambda i: (jnp.maximum(block_of(i) * (rows // HALO) - 1, 0), 0)
    )
    conv, swish_grad, sums, halo, taps8 = pl.pallas_call(
        functools.partial(forward_kernel, seqs, seq_blocks),
        grid=(blocks,),
        in_specs=[
            tile, tile, ahead_halo, ahead_halo, anywhere, anywhere,
            whole(conv_taps.shape),
            whole((1, chans)),
            pl.BlockSpec((rows, width), lambda i: (block_of(i), 0)),
            whole(out_weight.shape),
        ],
        out_specs=[tile, tile, whole(stats_shape), whole((seqs, HALO, chans)),
                   whole(taps_shape)],
        out_shape=[
            jax.ShapeDtypeStruct((positions, chans), F32),
            jax.ShapeDtypeStruct((positions, chans), F32),
            jax.ShapeDtypeStruct(stats_shape, F32),
            jax.ShapeDtypeStruct((seqs, HALO, chans), F32),
            jax.ShapeDtypeStruct(taps_shape, F32),
        ],
        scratch_shapes=[
            pltpu.VMEM((lane_blocks, rows + HALO, LANES), F32),
            pltpu.VMEM((seqs, HALO, chans), BF16),
            pltpu.VMEM((seqs, HALO, chans), BF16),
            dma(2),
            dma(2),
        ],
        compiler_params=params(0),
        name="forward",
    )(values, gates, values, gates, values_in, gates_in, conv_taps,
      conv_bias[None], cot, out_weight)

    ahead = pl.BlockSpec((rows, chans), lambda i: (jnp.minimum(i, blocks - 1), 0))
    normed_grad, back, gain_local, weight_local, stats = pl.pallas_call(
        functools.partial(middle_kernel, blocks, total_chans),
        grid=(blocks + 1,),
        in_specs=[
            ahead,
            ahead,
            whole(stats_shape),
            anywhere,
            whole((1, chans)),
            pl.BlockSpec((rows, width), lambda i: (jnp.maximum(i - 1, 0), 0)),
        ],
        out_specs=[
            ahead,
            whole(stats_shape),
            whole((8, chans)),
            whole((chans, width)),
            whole(stats_shape),
        ],
        out_shape=[
            jax.ShapeDtypeStruct((positions, chans), F32),
            jax.ShapeDtypeStruct(stats_shape, F32),
            jax.ShapeDtypeStruct((8, chans), F32),
            jax.ShapeDtypeStruct((chans, width), BF16),
            jax.ShapeDtypeStruct(stats_shape, F32),
        ],
        scratch_shapes=[
            pltpu.VMEM((2, chans, rows), BF16),
            pltpu.VMEM((chans, width), F32),
            pltpu.VMEM((tp_others, *stats_shape), F32),
            dma(tp_others),
            dma(tp_others),
        ],
        compiler_params=params(1),
        name="middle",
    )(conv, swish_grad, sums, sums, gain, cot)

    small_rows = -(-(K + 2) // 8) * 8
    weight_rows = chans // sp_devices
    groups = sp_devices // PAIR if sp_devices % PAIR == 0 else sp_devices
    padded_shape = (seqs * lane_blocks, tokens + HALO, LANES)
    values_grad, gates_grad, small, weight_grad = pl.pallas_call(
        functools.partial(backward_kernel, total_chans, seqs),
        in_specs=[anywhere] * 6 + [pl.BlockSpec(memory_space=pltpu.VMEM)] * 5,
        out_specs=[anywhere] * 2 + [pl.BlockSpec(memory_space=pltpu.VMEM)] * 2,
        out_shape=[
            jax.ShapeDtypeStruct((positions, chans), BF16),
            jax.ShapeDtypeStruct((positions, chans), BF16),
            jax.ShapeDtypeStruct((small_rows, chans), F32),
            jax.ShapeDtypeStruct((weight_rows, width), F32),
        ],
        scratch_shapes=[
            pltpu.VMEM((positions, chans), BF16),
            pltpu.VMEM((positions, chans), BF16),
            pltpu.VMEM((positions, chans), F32),
            pltpu.VMEM((positions, chans), F32),
            pltpu.VMEM(padded_shape, F32),
            pltpu.VMEM(padded_shape, F32),
            pltpu.VMEM((seqs * lane_blocks, HALO, LANES), F32),
            pltpu.VMEM(stats_shape, F32),
            pltpu.VMEM((tp_others, *stats_shape), F32),
            pltpu.VMEM((small_rows, chans), F32),
            pltpu.VMEM((sp_others, small_rows, chans), F32),
            pltpu.VMEM((groups, weight_rows, width), BF16),
            pltpu.VMEM((groups, weight_rows, width), BF16),
            pltpu.VMEM((max(groups - 1, 1), weight_rows, width), BF16),
            dma(seqs, 4),
            dma(seqs, 2),
            dma(groups),
            dma(groups),
            dma(groups),
            dma(tp_others),
            dma(tp_others),
            dma(max(groups - 1, 1)),
            dma(max(groups - 1, 1)),
            pltpu.SemaphoreType.DMA,
            pltpu.SemaphoreType.DMA,
            dma(sp_others),
            dma(sp_others),
        ],
        compiler_params=pltpu.CompilerParams(
            vmem_limit_bytes=VMEM_LIMIT, collective_id=2, has_side_effects=True
        ),
        name="backward",
    )(
        values, gates, conv, normed_grad,
        weight_local.reshape(sp_devices, weight_rows, width), back,
        halo, taps8, stats, back, gain_local,
    )
    return (
        values_grad.reshape(values_in.shape),
        gates_grad.reshape(values_in.shape),
        small[:K],
        small[K + 1],
        small[K],
        weight_grad,
    )


def solution(mesh):
    return jax.shard_map(
        on_device,
        mesh=mesh,
        in_specs=(
            P(None, "sp", "tp"),
            P(None, "sp", "tp"),
            P(None, "tp"),
            P("tp"),
            P("tp"),
            P("tp", None),
            P(None, "sp", None),
        ),
        out_specs=(
            P(None, "sp", "tp"),
            P(None, "sp", "tp"),
            P(None, "tp"),
            P("tp"),
            P("tp"),
            P(("tp", "sp"), None),
        ),
        check_vma=False,
    )
```
